256 devices in a mesh: sp: 64 (over z, x, core), tp: 4 (over y).
Axes of the slice: x: 4, y: 4, z: 8, core: 2. Of those that a mesh axis runs over, the one named last changes fastest.
Arguments:
- queries: bfloat16 [32768, 2048], P('sp', 'tp'), may hold values from -90 to 90, as said below
- key_rows: bfloat16 [32768, 512], P('sp', 'tp'), may hold values from -6 to 6
- value_rows: bfloat16 [32768, 512], P('sp', 'tp'), may hold values from -6 to 6
- sink_logits: float32 [16], P('tp'), may hold values from 2 to 7
- residual: bfloat16 [32768, 2048], P('sp'), may hold values from -6 to 6
- norm_gain: float32 [2048], replicated, may hold values from 0.1 to 1.9
- out_weight: bfloat16 [2048, 2048], P('tp'), may hold values from -1.5 to 1.5
- gate_weight: bfloat16 [2048, 5632], P('sp', 'tp'), may hold values from -0.125 to 0.125
- up_weight: bfloat16 [2048, 5632], P('sp', 'tp'), may hold values from -0.125 to 0.125
- down_weight: bfloat16 [5632, 2048], P('tp', 'sp'), may hold values from -0.078125 to 0.078125
Outputs:
- mixed: bfloat16 [32768, 2048], P(('sp', 'tp'))
The draws below stay inside these ranges and needn't reach their ends.
Inputs may be any that keep to these rules, and one draw needn't show every extreme that they name: queries are mostly of order one; some rows may be much larger.
All inputs are finite; a program needn't handle non-finite values.
Results may differ from the reference program's by a relative error of at most 0.012.
Values may be sent and summed in bfloat16 or wider, within the bound.
A program may use at most 128 MiB of HBM per device.

```python
import jax
import jax.numpy as jnp
from jax import lax

D = 2048
HQ = 16
HK = 4
DH = 128
FF = 5632
WIN = 128
TOKENS = 32768
N_TP = 4


def shared_draws(key):
    base = jax.random.fold_in(key, 11)
    key_query, key_keys = jax.random.split(base, 2)
    keys_wide = jnp.clip(jax.random.normal(key_keys, (TOKENS, HK * DH), jnp.float32), -5.0, 5.0)
    query_wide = jnp.clip(jax.random.normal(key_query, (TOKENS, HQ * DH), jnp.float32), -5.0, 5.0)
    return (query_wide, keys_wide)


def draw_queries(key, part):
    return shared_draws(key)[0].astype(jnp.bfloat16)


def draw_key_rows(key, part):
    return shared_draws(key)[1].astype(jnp.bfloat16)


def steps_of(stream_key, shape, cuts, smallest, largest):
    def one(position, shards_of):
        steps = jax.random.uniform(jax.random.fold_in(jax.random.fold_in(stream_key, 6), position), (shards_of,), jnp.float32, smallest / len(cuts), largest / len(cuts))
        return jnp.repeat(jnp.exp(steps), shape[position] // shards_of).reshape((-1,) + (1,) * (len(shape) - position - 1))

    factor_of = one(*cuts[0])
    for cut in cuts[1:]:
        factor_of = factor_of * one(*cut)
    return factor_of


def gaussian(stream_key, dims, spread, most, pieces=(), kind=jnp.bfloat16):
    level = steps_of(stream_key, dims, pieces, -0.22, 0.18) if pieces else 1.0
    values = jax.random.normal(stream_key, dims, jnp.float32) * spread * level
    return jnp.minimum(jnp.maximum(values, -most), most).astype(kind)


def setup_inputs(seed: int = 0) -> dict:
    key_of = jax.random.split(jax.random.key(seed), 11)
    return {
        "queries": draw_queries(jax.random.fold_in(key_of[10], 71), 0),
        "key_rows": draw_key_rows(jax.random.fold_in(key_of[10], 71), 0),
        "value_rows": gaussian(key_of[2], (TOKENS, HK * DH), 1.0, 6.0, ((0, 64), (1, 4))),
        "sink_logits": jnp.clip(2.0 + 5.0 * jax.random.uniform(key_of[3], (HQ,), jnp.float32) ** steps_of(key_of[3], (HQ,), ((0, 4),), -0.2, 0.2), 2.0, 7.0),
        "residual": gaussian(key_of[4], (TOKENS, D), 1.0, 6.0, ((0, 64),)),
        "norm_gain": jnp.clip(1.0 + 0.18 * jax.random.normal(key_of[5], (D,), jnp.float32), 0.1, 1.9),
        "out_weight": gaussian(key_of[6], (HQ * DH, D), 0.25, 1.5, ((0, 4),)),
        "gate_weight": gaussian(key_of[7], (D, FF), D ** -0.5, 0.125, ((0, 64), (1, 4))),
        "up_weight": gaussian(key_of[8], (D, FF), D ** -0.5, 0.125, ((0, 64), (1, 4))),
        "down_weight": gaussian(key_of[9], (FF, D), FF ** -0.5, 0.078125, ((0, 4), (1, 64))),
    }


EPSILON = 1e-06
MASKED = -1e+30

def attend_block(query_blk, key_blk, value_blk, sink_logits, query_pos, key_pos, seq_len):
    kv_heads = key_blk.shape[1] // DH
    group_size = query_blk.shape[1] // key_blk.shape[1]
    query_four = query_blk.reshape(query_blk.shape[0], kv_heads, group_size, DH).astype(jnp.float32)
    key_three = key_blk.reshape(key_blk.shape[0], kv_heads, DH).astype(jnp.float32)
    value_three = value_blk.reshape(value_blk.shape[0], kv_heads, DH).astype(jnp.float32)
    scores = jnp.einsum('qhgd,khd->hgqk', query_four, key_three) * DH ** (-0.5)
    allowed = (jnp.abs(key_pos[None, :] - query_pos[:, None]) <= WIN) & (key_pos[None, :] >= 0) & (key_pos[None, :] < seq_len)
    scores = jnp.where(allowed[None, None], scores, MASKED)
    sink_col = sink_logits.astype(jnp.float32).reshape(kv_heads, group_size)[:, :, None]
    highest = jnp.maximum(lax.optimization_barrier(jnp.max(scores, axis=-1)), sink_col)
    weights_exp = jnp.exp(scores - highest[..., None])
    denominator = lax.optimization_barrier(jnp.sum(weights_exp, axis=-1)) + jnp.exp(sink_col - highest)
    probabilities = (weights_exp / denominator[..., None]).astype(jnp.bfloat16)
    heads_out = jnp.einsum('hgqk,khd->qhgd', probabilities.astype(jnp.float32), value_three)
    return heads_out.astype(jnp.bfloat16).reshape(query_blk.shape[0], kv_heads * group_size * DH)

def rms_scale(rows_wide, norm_gain):
    mean_square = lax.optimization_barrier(jnp.mean(rows_wide * rows_wide, axis=-1, keepdims=True))
    return (rows_wide * lax.rsqrt(mean_square + EPSILON) * norm_gain).astype(jnp.bfloat16)

def grouped_sum(left, right, group_cols):
    result = jnp.zeros((left.shape[0], right.shape[1]), jnp.float32)
    for group_index in range(N_TP):
        lower = group_index * group_cols
        partial_term = jnp.dot(left[:, lower:lower + group_cols], right[lower:lower + group_cols], preferred_element_type=jnp.float32)
        rounded = lax.optimization_barrier(partial_term.astype(jnp.bfloat16))
        result = result + rounded.astype(jnp.float32)
    return result

def reference(queries, key_rows, value_rows, sink_logits, residual, norm_gain, out_weight, gate_weight, up_weight, down_weight):
    block_len = 2 * WIN
    key_pad = jnp.pad(key_rows, ((WIN, WIN), (0, 0)))
    value_pad = jnp.pad(value_rows, ((WIN, WIN), (0, 0)))

    def one_block(block_index):
        block_first = (block_index * block_len).astype(jnp.int32)
        query_blk = lax.dynamic_slice_in_dim(queries, block_first, block_len, 0)
        key_blk = lax.dynamic_slice_in_dim(key_pad, block_first, block_len + 2 * WIN, 0)
        value_blk = lax.dynamic_slice_in_dim(value_pad, block_first, block_len + 2 * WIN, 0)
        query_pos = block_first + jnp.arange(block_len, dtype=jnp.int32)
        key_pos = block_first - WIN + jnp.arange(block_len + 2 * WIN, dtype=jnp.int32)
        return attend_block(query_blk, key_blk, value_blk, sink_logits, query_pos, key_pos, TOKENS)
    blocks = lax.map(one_block, jnp.arange(TOKENS // block_len, dtype=jnp.int32))
    attended = blocks.reshape(TOKENS, HQ * DH)
    attn_total = grouped_sum(attended, out_weight, HQ * DH // N_TP)
    middle = residual.astype(jnp.float32) + attn_total
    normed = rms_scale(middle, norm_gain)
    gate_acc = jnp.dot(normed, gate_weight, preferred_element_type=jnp.float32)
    up_acc = jnp.dot(normed, up_weight, preferred_element_type=jnp.float32)
    hidden = (jax.nn.silu(gate_acc) * up_acc).astype(jnp.bfloat16)
    ffn_total = grouped_sum(hidden, down_weight, FF // N_TP)
    return (middle + ffn_total).astype(jnp.bfloat16)
```

```python
import functools

import jax
import jax.numpy as jnp
from jax import lax
from jax.experimental import pallas as pl
from jax.experimental.pallas import tpu as pltpu
from jax.sharding import PartitionSpec as P

DH = 128
WIN = 128
EPSILON = 1e-06
MASKED = -1e30
ZN, XN, CN = 8, 4, 2
MESH = pl.DeviceIdType.MESH
F32 = jnp.float32
BF16 = jnp.bfloat16
N_COPIES = 192
FIRST_CHUNKS = 4
LAST_CHUNKS = 8


def body(
    seq_len,
    q_ref,
    k_ref,
    v_ref,
    sink_ref,
    res_hbm,
    gain_ref,
    wo_hbm,
    g_ref,
    u_ref,
    d_ref,
    out_ref,
    kbuf,
    vbuf,
    res_ref,
    wo_ref,
    gate,
    up,
    down,
    att,
    first,
    first_relay,
    first_in,
    middle,
    normed,
    hidden,
    last,
    last_relay,
    last_in,
    send_sems,
    recv_sems,
    local_sems,
):
    sp = lax.axis_index("sp")
    y = lax.axis_index("tp")
    n_sp = lax.axis_size("sp")
    c = lax.rem(sp, CN)
    x = lax.rem(lax.div(sp, CN), XN)
    z = lax.div(sp, CN * XN)
    tok = q_ref.shape[0]
    share = tok // 4
    half = share // 2

    def at_z(k):
        return lax.rem(z + (k + ZN), ZN)

    def spot(zz, xx, cc):
        return {"sp": (zz * XN + xx) * CN + cc, "tp": y}

    z_up, z_down = spot(at_z(1), x, c), spot(at_z(-1), x, c)
    x_up = spot(z, lax.rem(x + 1, XN), c)
    x_down = spot(z, lax.rem(x + XN - 1, XN), c)
    twin = spot(z, x, 1 - c)
    y_up = {"sp": sp, "tp": lax.rem(y + 1, 4)}
    y_down = {"sp": sp, "tp": lax.rem(y + 3, 4)}
    y_far = lax.rem(y + 2, 4)
    right = {"sp": lax.rem(sp + 1, n_sp), "tp": y}
    left = {"sp": lax.rem(sp + n_sp - 1, n_sp), "tp": y}

    sent = []

    def push(src, dst, device):
        i = len(sent)
        copy = pltpu.make_async_remote_copy(
            src_ref=src,
            dst_ref=dst,
            send_sem=send_sems.at[i],
            recv_sem=recv_sems.at[i],
            device_id=device,
            device_id_type=MESH,
        )
        copy.start()
        sent.append(copy)
        return copy

    def local(i, src, dst):
        copy = pltpu.make_async_copy(src, dst, local_sems.at[i])
        copy.start()
        return copy

    wo_copy = local(0, wo_hbm, wo_ref)
    res_copy = local(1, res_hbm.at[pl.ds(pl.multiple_of(y * share, share), share)], res_ref)
    k_copy = local(2, k_ref, kbuf.at[pl.ds(WIN, tok)])
    v_copy = local(3, v_ref, vbuf.at[pl.ds(WIN, tok)])
    own = {
        "g": local(4, g_ref, gate.at[z, x, c]),
        "u": local(5, u_ref, up.at[z, x, c]),
        "d": local(6, d_ref, down.at[z, x, c]),
    }

    barrier = pltpu.get_barrier_semaphore()
    peers = (x_up, x_down, z_up, z_down, twin, y_up, y_down, left, right)
    for peer in peers:
        pl.semaphore_signal(barrier, inc=1, device_id=peer, device_id_type=MESH)
    pl.semaphore_wait(barrier, len(peers))

    buffers = {"u": (u_ref, up), "d": (d_ref, down)}
    spots = (0, -1, 1, -2, 2, -3, 3, 4)
    on_z, on_x, relayed, gate_x, gate_z, twins = {}, {}, {}, {}, {}, {"g": [], "u": [], "d": []}
    lo, hi = pl.ds(0, 16), pl.ds(16, 16)

    def halo():
        return (
            push(k_ref.at[pl.ds(tok - WIN, WIN)], kbuf.at[pl.ds(0, WIN)], right),
            push(v_ref.at[pl.ds(tok - WIN, WIN)], vbuf.at[pl.ds(0, WIN)], right),
            push(k_ref.at[pl.ds(0, WIN)], kbuf.at[pl.ds(WIN + tok, WIN)], left),
            push(v_ref.at[pl.ds(0, WIN)], vbuf.at[pl.ds(WIN + tok, WIN)], left),
        )

    def to_twin(name, ref):
        twins[name].append(push(ref, ref, twin))

    def start_z(m):
        source, buf = buffers[m]
        on_z[m, "u", 1] = push(source, buf.at[z, x, c], z_up)
        on_z[m, "d", 1] = push(source, buf.at[z, x, c], z_down)

    def send_x(m, j):
        source, buf = buffers[m]
        k = spots[j]
        zz = at_z(k)
        block = buf.at[zz, x, c]
        if k == 4:
            on_z[m, "u", 4].wait_recv()
            on_z[m, "d", 4].wait_recv()
        elif k:
            way, n = ("u" if k < 0 else "d"), abs(k)
            on_z[m, way, n].wait_recv()
            passed = block if n < 3 else block.at[lo if way == "u" else hi]
            on_z[m, way, n + 1] = push(passed, passed, z_up if way == "u" else z_down)
        source = block if k else source
        on_x[m, j, "u"] = push(source, block, x_up)
        on_x[m, j, "d"] = push(source, block, x_down)

    def relay_x(m, j):
        buf = buffers[m][1]
        zz = at_z(spots[j])
        on_x[m, j, "u"].wait_recv()
        part = buf.at[zz, lax.rem(x + XN - 1, XN), c, lo]
        relayed[m, j, "u"] = push(part, part, x_up)
        on_x[m, j, "d"].wait_recv()
        part = buf.at[zz, lax.rem(x + 1, XN), c, hi]
        relayed[m, j, "d"] = push(part, part, x_down)

    def close_x(m, j):
        if j == 0:
            own[m].wait()
        relayed[m, j, "u"].wait_recv()
        relayed[m, j, "d"].wait_recv()
        to_twin(m, buffers[m][1].at[at_z(spots[j]), :, c])

    def gate_start():
        gate_x["u"] = push(g_ref, gate.at[z, x, c], x_up)
        gate_x["d"] = push(g_ref, gate.at[z, x, c], x_down)

    def gate_relay():
        gate_x["u"].wait_recv()
        part = gate.at[z, lax.rem(x + XN - 1, XN), c, lo]
        gate_x["ru"] = push(part, part, x_up)
        gate_x["d"].wait_recv()
        part = gate.at[z, lax.rem(x + 1, XN), c, hi]
        gate_x["rd"] = push(part, part, x_down)

    def gate_turn():
        own["g"].wait()
        gate_x["ru"].wait_recv()
        gate_x["rd"].wait_recv()
        bundle = gate.at[z, :, c]
        gate_z["u", 1] = push(bundle, bundle, z_up)
        gate_z["d", 1] = push(bundle, bundle, z_down)
        to_twin("g", bundle)

    def gate_step(k):
        if k == 4:
            gate_z["u", 4].wait_recv()
            gate_z["d", 4].wait_recv()
            to_twin("g", gate.at[at_z(4), :, c])
            return
        for way, zz, to in (("u", at_z(-k), z_up), ("d", at_z(k), z_down)):
            gate_z[way, k].wait_recv()
            bundle = gate.at[zz, :, c]
            if k < 3:
                passed = bundle
            else:
                passed = gate.at[zz, pl.ds(0 if way == "u" else 2, 2), c]
            gate_z[way, k + 1] = push(passed, passed, to)
            to_twin("g", bundle)

    offset = sp * tok

    def attend(b):
        keys = kbuf[pl.ds(b * share, share + 2 * WIN), :]
        values = vbuf[pl.ds(b * share, share + 2 * WIN), :]
        span = share + 2 * WIN
        row = lax.broadcasted_iota(jnp.int32, (share, span), 0)
        col = lax.broadcasted_iota(jnp.int32, (share, span), 1)
        gap = col - row
        place = col + (offset + (b * share - WIN))
        kept = (gap >= 0) & (gap <= 2 * WIN) & (place >= 0) & (place < seq_len)
        for h in range(q_ref.shape[1] // DH):
            query = q_ref[pl.ds(b * share, share), pl.ds(h * DH, DH)]
            score = lax.dot_general(
                query, keys, (((1,), (1,)), ((), ())), preferred_element_type=F32
            ) * DH ** (-0.5)
            score = jnp.where(kept, score, MASKED)
            sink = sink_ref[h]
            top = jnp.maximum(jnp.max(score, axis=-1, keepdims=True), sink)
            weight = jnp.exp(score - top)
            total = jnp.sum(weight, axis=-1, keepdims=True) + jnp.exp(sink - top)
            prob = (weight * (1.0 / total)).astype(BF16)
            att[pl.ds(b * share, share), pl.ds(h * DH, DH)] = jnp.dot(
                prob, values, preferred_element_type=F32
            ).astype(BF16)

    def sum_send(n, part, relay, steps):
        steps[n, "ru"] = push(part.at[n, y_far, pl.ds(0, half)], relay.at[0, n], y_up)
        steps[n, "rd"] = push(part.at[n, y_far, pl.ds(half, half)], relay.at[1, n], y_down)

    def sum_pass(n, part, relay, arrived, steps):
        steps[n, "ru"].wait_recv()
        to = lax.rem(y + 1, 4)
        part[n, to, pl.ds(0, half)] = (
            part[n, to, pl.ds(0, half)].astype(F32) + relay[0, n].astype(F32)
        ).astype(BF16)
        steps[n, "u"] = push(part.at[n, to], arrived.at[0, n], y_up)
        steps[n, "rd"].wait_recv()
        to = lax.rem(y + 3, 4)
        part[n, to, pl.ds(half, half)] = (
            part[n, to, pl.ds(half, half)].astype(F32) + relay[1, n].astype(F32)
        ).astype(BF16)
        steps[n, "d"] = push(part.at[n, to], arrived.at[1, n], y_down)

    def sum_take(n, part, arrived, steps):
        steps[n, "u"].wait_recv()
        steps[n, "d"].wait_recv()
        return part[n, y].astype(F32) + arrived[0, n].astype(F32) + arrived[1, n].astype(F32)

    first_steps, last_steps = {}, {}
    width = wo_ref.shape[1] // FIRST_CHUNKS

    def project(n):
        product = jnp.dot(att[...], wo_ref[:, pl.ds(n * width, width)], preferred_element_type=F32)
        first[n] = product.astype(BF16).reshape(4, share, width)
        sum_send(n, first, first_relay, first_steps)

    def pass_first(n):
        sum_pass(n, first, first_relay, first_in, first_steps)

    spread = {}

    def norm():
        res_copy.wait()
        squares = jnp.zeros((share, 1), F32)
        for n in range(FIRST_CHUNKS):
            cols = pl.ds(n * width, width)
            rows = res_ref[:, cols].astype(F32) + sum_take(n, first, first_in, first_steps)
            middle[:, cols] = rows
            squares += jnp.sum(rows * rows, axis=-1, keepdims=True)
        scale = lax.rsqrt(squares * (1.0 / middle.shape[1]) + EPSILON)
        for n in range(FIRST_CHUNKS):
            cols = pl.ds(n * width, width)
            normed[y, :, cols] = (middle[:, cols] * scale * gain_ref[:, cols]).astype(BF16)
        top, low = normed.at[y, pl.ds(0, half)], normed.at[y, pl.ds(half, half)]
        spread["u0"] = push(top, top, y_up)
        spread["d1"] = push(low, low, y_down)
        spread["u1"] = push(low, low, y_up)
        spread["d0"] = push(top, top, y_down)

    def spread_relay():
        spread["u0"].wait_recv()
        part = normed.at[lax.rem(y + 3, 4), pl.ds(0, half)]
        spread["ru"] = push(part, part, y_up)
        spread["d1"].wait_recv()
        part = normed.at[lax.rem(y + 1, 4), pl.ds(half, half)]
        spread["rd"] = push(part, part, y_down)

    def spread_end():
        for name in ("u1", "d0", "ru", "rd"):
            spread[name].wait_recv()

    rows_in = middle.shape[1]

    def expand_cols(cols):
        tokens = normed[...].reshape(tok, rows_in)
        g_acc = jnp.dot(
            tokens, gate[:, :, :, :, cols].reshape(rows_in, cols.size), preferred_element_type=F32
        )
        u_acc = jnp.dot(
            tokens, up[:, :, :, :, cols].reshape(rows_in, cols.size), preferred_element_type=F32
        )
        hidden[:, cols] = (g_acc / (1.0 + jnp.exp(-g_acc)) * u_acc).astype(BF16)

    def expand(first_tile, tiles):
        def step(t, carry):
            expand_cols(pl.ds(pl.multiple_of(t * 256, 256), 256))
            return carry

        lax.fori_loop(first_tile, first_tile + tiles, step, 0)

    def contract(j):
        block = down[at_z(spots[j])].reshape(256, hidden.shape[1])
        product = lax.dot_general(
            hidden[...], block, (((1,), (1,)), ((), ())), preferred_element_type=F32
        )
        last[j] = product.astype(BF16).reshape(4, share, 256)
        sum_send(j, last, last_relay, last_steps)

    def pass_last(j):
        sum_pass(j, last, last_relay, last_in, last_steps)

    def finish(j):
        total = sum_take(j, last, last_in, last_steps)
        cols = pl.ds(pl.multiple_of(at_z(spots[j]) * 256, 256), 256)
        out_ref[:, cols] = (middle[:, cols] + total).astype(BF16)

    halos = halo()
    gate_start()
    start_z("u")
    send_x("u", 0)
    start_z("d")
    k_copy.wait()
    v_copy.wait()
    attend(1)
    gate_relay()
    send_x("u", 1)
    send_x("u", 2)
    attend(2)
    relay_x("u", 0)
    gate_turn()
    for copy in halos:
        copy.wait_recv()
    attend(0)
    send_x("u", 3)
    send_x("u", 4)
    attend(3)
    relay_x("u", 1)
    wo_copy.wait()
    project(0)
    project(1)
    send_x("u", 5)
    send_x("u", 6)
    project(2)
    project(3)
    close_x("u", 0)
    relay_x("u", 2)
    send_x("u", 7)
    send_x("d", 0)
    pass_first(0)
    close_x("u", 1)
    relay_x("u", 3)
    pass_first(1)
    send_x("d", 1)
    close_x("u", 2)
    relay_x("u", 4)
    pass_first(2)
    gate_step(1)
    send_x("d", 2)
    close_x("u", 3)
    relay_x("u", 5)
    pass_first(3)
    send_x("d", 3)
    close_x("u", 4)
    relay_x("u", 6)
    send_x("d", 4)
    close_x("u", 5)
    relay_x("u", 7)
    gate_step(2)
    send_x("d", 5)
    close_x("u", 6)
    relay_x("d", 0)
    norm()
    send_x("d", 6)
    close_x("u", 7)
    relay_x("d", 1)
    send_x("d", 7)
    close_x("d", 0)
    relay_x("d", 2)
    gate_step(3)
    close_x("d", 1)
    relay_x("d", 3)
    spread_relay()
    close_x("d", 2)
    relay_x("d", 4)
    close_x("d", 3)
    relay_x("d", 5)
    gate_step(4)
    for copy in twins["g"] + twins["u"]:
        copy.wait_recv()
    spread_end()
    expand(0, 2)
    close_x("d", 4)
    relay_x("d", 6)
    expand(2, 2)
    close_x("d", 5)
    relay_x("d", 7)
    expand(4, 1)
    expand_cols(pl.ds(1280, 128))
    close_x("d", 6)
    close_x("d", 7)
    for j in range(LAST_CHUNKS):
        twins["d"][j].wait_recv()
        contract(j)
        if j >= 2:
            pass_last(j - 2)
    pass_last(LAST_CHUNKS - 2)
    pass_last(LAST_CHUNKS - 1)
    for j in range(LAST_CHUNKS):
        finish(j)
    for copy in sent:
        copy.wait_send()


def shards(
    queries,
    key_rows,
    value_rows,
    sink_logits,
    residual,
    norm_gain,
    out_weight,
    gate_weight,
    up_weight,
    down_weight,
):
    tok, width = queries.shape
    d = residual.shape[1]
    rows, ff = gate_weight.shape
    share = tok // 4
    whole = pltpu.VMEM((ZN, XN, CN, rows, ff), BF16)
    wide, narrow = d // FIRST_CHUNKS, d // LAST_CHUNKS
    vmem = pl.BlockSpec(memory_space=pltpu.VMEM)
    hbm = pl.BlockSpec(memory_space=pl.ANY)
    smem = pl.BlockSpec(memory_space=pltpu.SMEM)
    return pl.pallas_call(
        functools.partial(body, tok * lax.axis_size("sp")),
        out_shape=jax.ShapeDtypeStruct((share, d), BF16),
        in_specs=[vmem, vmem, vmem, smem, hbm, vmem, hbm, vmem, vmem, vmem],
        out_specs=vmem,
        scratch_shapes=[
            pltpu.VMEM((tok + 2 * WIN, DH), BF16),
            pltpu.VMEM((tok + 2 * WIN, DH), BF16),
            pltpu.VMEM((share, d), BF16),
            pltpu.VMEM((width, d), BF16),
            whole,
            whole,
            whole,
            pltpu.VMEM((tok, width), BF16),
            pltpu.VMEM((FIRST_CHUNKS, 4, share, wide), BF16),
            pltpu.VMEM((2, FIRST_CHUNKS, share // 2, wide), BF16),
            pltpu.VMEM((2, FIRST_CHUNKS, share, wide), BF16),
            pltpu.VMEM((share, d), F32),
            pltpu.VMEM((4, share, d), BF16),
            pltpu.VMEM((tok, ff), BF16),
            pltpu.VMEM((LAST_CHUNKS, 4, share, narrow), BF16),
            pltpu.VMEM((2, LAST_CHUNKS, share // 2, narrow), BF16),
            pltpu.VMEM((2, LAST_CHUNKS, share, narrow), BF16),
            pltpu.SemaphoreType.DMA((N_COPIES,)),
            pltpu.SemaphoreType.DMA((N_COPIES,)),
            pltpu.SemaphoreType.DMA((7,)),
        ],
        compiler_params=pltpu.CompilerParams(
            collective_id=0, has_side_effects=True, vmem_limit_bytes=67043328
        ),
        name="layer",
    )(
        queries,
        key_rows,
        value_rows,
        sink_logits,
        residual,
        norm_gain.reshape(1, d),
        out_weight,
        gate_weight,
        up_weight,
        down_weight.T,
    )


def solution(mesh):
    placed = (
        P("sp", "tp"),
        P("sp", "tp"),
        P("sp", "tp"),
        P("tp"),
        P("sp", None),
        P(),
        P("tp", None),
        P("sp", "tp"),
        P("sp", "tp"),
        P("tp", "sp"),
    )
    return jax.shard_map(
        shards, mesh=mesh, in_specs=placed, out_specs=P(("sp", "tp"), None), check_vma=False
    )
```

```python
import functools

import jax
import jax.numpy as jnp
from jax import lax
from jax.experimental import pallas as pl
from jax.experimental.pallas import tpu as pltpu
from jax.sharding import PartitionSpec as P

DH = 128
WIN = 128
EPSILON = 1e-06
MASKED = -1e30
ZN, XN, CN = 8, 4, 2
MESH = pl.DeviceIdType.MESH
F32 = jnp.float32
BF16 = jnp.bfloat16
N_SENT, N_ARRIVING = 31, 90
LAST_CHUNKS = 8


def body(
    seq_len,
    q_hbm,
    k_hbm,
    v_hbm,
    sink_ref,
    res_hbm,
    gain_hbm,
    wo_hbm,
    g_hbm,
    u_hbm,
    d_hbm,
    out_ref,
    q_ref,
    kbuf,
    vbuf,
    res_ref,
    gain_ref,
    wo_ref,
    gate,
    up,
    down,
    att,
    first,
    first_relay,
    first_in,
    middle,
    normed,
    up_acc,
    hidden,
    last,
    last_relay,
    last_in,
    send_sems,
    recv_sems,
    local_sems,
):
    sp = lax.axis_index("sp")
    y = lax.axis_index("tp")
    n_sp = lax.axis_size("sp")
    c = lax.rem(sp, CN)
    x = lax.rem(lax.div(sp, CN), XN)
    z = lax.div(sp, CN * XN)
    tok = q_ref.shape[0]
    share = tok // 4
    half = share // 2
    top, low = pl.ds(0, half), pl.ds(half, half)

    def at_z(k):
        return lax.rem(z + (k + ZN), ZN)

    def at_x(k):
        return lax.rem(x + (k + XN), XN)

    def spot(zz, xx, cc):
        return {"sp": (zz * XN + xx) * CN + cc, "tp": y}

    z_up, z_down = spot(at_z(1), x, c), spot(at_z(-1), x, c)
    x_up, x_down = spot(z, at_x(1), c), spot(z, at_x(-1), c)
    twin = spot(z, x, 1 - c)
    y_up = {"sp": sp, "tp": lax.rem(y + 1, 4)}
    y_down = {"sp": sp, "tp": lax.rem(y + 3, 4)}
    right = {"sp": lax.rem(sp + 1, n_sp), "tp": y}
    left = {"sp": lax.rem(sp + n_sp - 1, n_sp), "tp": y}

    lo, hi = pl.ds(0, 16), pl.ds(16, 16)
    sent, arriving = [], {}
    kinds = {
        "block": (8, lambda n: gate.at[pl.ds(0, n), 0, 0]),
        "part": (8, lambda n: gate.at[pl.ds(0, n), 0, 0, lo]),
        "bundle": (8, lambda n: gate.at[pl.ds(0, n), :, 0]),
        "halo": (4, lambda n: kbuf.at[pl.ds(0, n * WIN)]),
        "rows": (2, lambda n: first.at[0, pl.ds(0, n * half)]),
        "cols": (8, lambda n: last.at[pl.ds(0, n), 0, top]),
    }

    def push(kind, key, src, dst, device):
        groups = [i for i, (of, n) in enumerate(sent) if of == kind and n < kinds[kind][0]]
        if groups:
            i = groups[0]
            sent[i] = (kind, sent[i][1] + 1)
        else:
            i = len(sent)
            sent.append((kind, 1))
        pltpu.make_async_remote_copy(
            src_ref=src,
            dst_ref=dst,
            send_sem=send_sems.at[i],
            recv_sem=recv_sems.at[arriving.setdefault(key, len(arriving))],
            device_id=device,
            device_id_type=MESH,
        ).start()

    def wait_bytes(sem, ref):
        pltpu.make_async_copy(ref, ref, sem).wait()

    def take(key, kind, n):
        wait_bytes(recv_sems.at[arriving[key]], kinds[kind][1](n))

    def wait_sent():
        for i, (kind, n) in enumerate(sent):
            wait_bytes(send_sems.at[i], kinds[kind][1](n))

    def local(i, src, dst):
        copy = pltpu.make_async_copy(src, dst, local_sems.at[i])
        copy.start()
        return copy

    k_copy = local(0, k_hbm, kbuf.at[pl.ds(WIN, tok)])
    v_copy = local(1, v_hbm, vbuf.at[pl.ds(WIN, tok)])
    own_up = local(2, u_hbm, up.at[z, x, c])
    own_gate = local(3, g_hbm, gate.at[z, x, c])
    own_down = local(4, d_hbm, down.at[z, x, c])
    q_copy = local(5, q_hbm, q_ref)
    wo_copy = local(6, wo_hbm, wo_ref)
    res_copy = local(7, res_hbm.at[pl.ds(pl.multiple_of(y * share, share), share)], res_ref)
    gain_copy = local(8, gain_hbm, gain_ref)

    barrier = pltpu.get_barrier_semaphore()
    peers = (x_up, x_down, z_up, z_down, twin, y_up, y_down, left, right)
    for peer in peers:
        pl.semaphore_signal(barrier, inc=1, device_id=peer, device_id_type=MESH)
    pl.semaphore_wait(barrier, len(peers))

    buffers = {"u": up, "d": down}
    spots = (0, -1, 1, -2, 2, -3, 3, 4)

    def halo():
        k_copy.wait()
        v_copy.wait()
        for start, to, device in ((tok, 0, right), (WIN, WIN + tok, left)):
            for ref in (kbuf, vbuf):
                push("halo", "halo", ref.at[pl.ds(start, WIN)], ref.at[pl.ds(to, WIN)], device)

    def wait_halos():
        take("halo", "halo", 4)

    def to_twin(key, ref):
        push("bundle", key, ref, ref, twin)

    def hop(flow, k, block, halves):
        if k:
            take((flow, k), "block", 2 if k < 4 else 1)
        if k < 4:
            for way, zz, to in ((0, at_z(-k), z_up), (1, at_z(k), z_down)):
                ref = block(zz)
                if k == 3:
                    ref = ref.at[halves[way]]
                push("block" if k < 3 else "part", (flow, k + 1), ref, ref, to)

    def z_hop(m, k):
        hop(m, k, lambda zz: buffers[m].at[zz, x, c], (lo, hi))

    def gate_hop(i, k):
        hop(i, k, lambda zz: gate.at[zz, at_x(i), c], (lo, hi))

    def gate_twin(k):
        for kk in sorted({-k, k if k < 4 else -k}):
            to_twin("gt", gate.at[at_z(kk), :, c])

    def along_x(key, block):
        push("block", key, block, block, x_up)
        push("block", key, block, block, x_down)

    def relay_along_x(key, later, line):
        take(key, "block", 2)
        for part, to in ((line.at[at_x(-1), c, lo], x_up), (line.at[at_x(1), c, hi], x_down)):
            push("part", later, part, part, to)

    def send_x(m, j):
        along_x(("x", m, j), buffers[m].at[at_z(spots[j]), x, c])

    def relay_x(m, j):
        relay_along_x(("x", m, j), ("r", m, j), buffers[m].at[at_z(spots[j])])

    def close_x(m, j):
        take(("r", m, j), "block", 1)
        to_twin("ut" if m == "u" else ("dt", j), buffers[m].at[at_z(spots[j]), :, c])

    def gate_start():
        along_x("gx", gate.at[z, x, c])

    def gate_relay():
        relay_along_x("gx", "gr", gate.at[z])

    def gate_close():
        take("gr", "block", 1)

    def wait_twins(name):
        take(name + "t", "bundle", 8)

    offset = sp * tok
    shares = {0: y, 1: lax.rem(y + 1, 4), 2: lax.rem(y + 3, 4), 3: lax.rem(y + 2, 4)}
    late = lax.div(y, 2)
    inner = lax.rem(lax.div(y + 1, 2), 2)

    def attend(b):
        start = pl.multiple_of(b * share, share)
        span = share + 2 * WIN
        keys = kbuf[pl.ds(start, span), :]
        values = vbuf[pl.ds(start, span), :]
        row = lax.broadcasted_iota(jnp.int32, (share, span), 0)
        col = lax.broadcasted_iota(jnp.int32, (share, span), 1)
        gap = col - row
        place = col + (offset + start - WIN)
        kept = (gap >= 0) & (gap <= 2 * WIN) & (place >= 0) & (place < seq_len)
        for h in range(q_ref.shape[1] // DH):
            query = q_ref[pl.ds(start, share), pl.ds(h * DH, DH)]
            score = lax.dot_general(
                query, keys, (((1,), (1,)), ((), ())), preferred_element_type=F32
            ) * DH ** (-0.5)
            score = jnp.where(kept, score, MASKED)
            sink = sink_ref[h]
            most = jnp.maximum(jnp.max(score, axis=-1, keepdims=True), sink)
            weight = jnp.exp(score - most)
            total = jnp.sum(weight, axis=-1, keepdims=True) + jnp.exp(sink - most)
            prob = (weight * (1.0 / total)).astype(BF16)
            att[pl.ds(start, share), pl.ds(h * DH, DH)] = jnp.dot(
                prob, values, preferred_element_type=F32
            ).astype(BF16)

    def attend_early():
        attend(lax.rem(y + 1 + 2 * late, 4))

    def attend_second():
        attend(lax.rem(y + 2 * (1 - inner), 4))

    def attend_third():
        attend(lax.rem(y + 2 * inner, 4))

    def attend_late():
        attend(lax.rem(y + 3 + 2 * late, 4))

    def project(place):
        start = pl.multiple_of(shares[place] * share, share)
        first[place] = jnp.dot(
            att[pl.ds(start, share), :], wo_ref[...], preferred_element_type=F32
        ).astype(BF16)
        if place == 3:
            push("rows", "far", first.at[3, top], first_relay.at[0], y_up)
            push("rows", "far", first.at[3, low], first_relay.at[1], y_down)
        elif place == 1:
            push("rows", "near", first.at[1, low], first_in.at[0, low], y_up)
        elif place == 2:
            push("rows", "near", first.at[2, top], first_in.at[1, top], y_down)

    def pass_first():
        take("far", "rows", 2)
        first[1, top] = (first[1, top].astype(F32) + first_relay[0].astype(F32)).astype(BF16)
        push("rows", "near", first.at[1, top], first_in.at[0, top], y_up)
        first[2, low] = (first[2, low].astype(F32) + first_relay[1].astype(F32)).astype(BF16)
        push("rows", "near", first.at[2, low], first_in.at[1, low], y_down)

    rows_in = middle.shape[1]

    def norm():
        res_copy.wait()
        gain_copy.wait()
        wait_bytes(recv_sems.at[arriving["near"]], first.at[pl.ds(0, 2)])
        squares = jnp.zeros((share, 1), F32)
        width = 512
        for n in range(rows_in // width):
            cols = pl.ds(n * width, width)
            rows = res_ref[:, cols].astype(F32) + (
                first[0, :, cols].astype(F32)
                + first_in[0, :, cols].astype(F32)
                + first_in[1, :, cols].astype(F32)
            )
            middle[:, cols] = rows
            squares += jnp.sum(rows * rows, axis=-1, keepdims=True)
        scale = lax.rsqrt(squares * (1.0 / rows_in) + EPSILON)
        for n in range(rows_in // width):
            cols = pl.ds(n * width, width)
            normed[0, :, cols] = (middle[:, cols] * scale * gain_ref[:, cols]).astype(BF16)
        push("rows", "s0", normed.at[0, top], normed.at[2, top], y_up)
        push("rows", "s0", normed.at[0, low], normed.at[1, low], y_down)
        push("rows", "s1", normed.at[0, low], normed.at[2, low], y_up)
        push("rows", "s1", normed.at[0, top], normed.at[1, top], y_down)

    def spread_relay():
        take("s0", "rows", 2)
        push("rows", "s2", normed.at[2, top], normed.at[3, top], y_up)
        push("rows", "s2", normed.at[1, low], normed.at[3, low], y_down)

    def spread_near():
        take("s1", "rows", 2)

    def spread_far():
        take("s2", "rows", 2)

    def over_tiles(tile, first_tile, tiles, rest):
        def step(t, carry):
            tile(pl.ds(pl.multiple_of(t * 256, 256), 256))
            return carry

        lax.fori_loop(first_tile, first_tile + tiles, step, 0)
        if rest:
            tile(pl.ds(1280, 128))

    def times(weight, place, count, cols):
        return jnp.dot(
            normed[pl.ds(place, count)].reshape(count * share, rows_in),
            weight[:, :, :, :, cols].reshape(rows_in, cols.size),
            preferred_element_type=F32,
        )

    def expand_up(place, count, first_tile, tiles, rest=False):
        def tile(cols):
            up_acc[pl.ds(place * share, count * share), cols] = times(up, place, count, cols)

        over_tiles(tile, first_tile, tiles, rest)

    def expand_gate(place, count, first_tile, tiles, rest=False):
        def tile(cols):
            rows = pl.ds(place * share, count * share)
            g_acc = times(gate, place, count, cols)
            hidden[rows, cols] = (g_acc / (1.0 + jnp.exp(-g_acc)) * up_acc[rows, cols]).astype(BF16)

        over_tiles(tile, first_tile, tiles, rest)

    def contract(j, place, count):
        product = lax.dot_general(
            hidden[pl.ds(place * share, count * share)],
            down[at_z(spots[j])].reshape(256, hidden.shape[1]),
            (((1,), (1,)), ((), ())),
            preferred_element_type=F32,
        )
        last[j, pl.ds(place, count)] = product.astype(BF16).reshape(count, share, 256)

    def send_near(j):
        push("cols", ("e", j), last.at[j, 1, low], last_in.at[0, j, low], y_up)
        push("cols", ("e", j), last.at[j, 2, top], last_in.at[1, j, top], y_down)

    def send_far(j):
        push("cols", ("f", j), last.at[j, 3, top], last_relay.at[0, j], y_up)
        push("cols", ("f", j), last.at[j, 3, low], last_relay.at[1, j], y_down)

    def contract_near(j):
        take(("dt", j), "bundle", 1)
        contract(j, 0, 3)
        send_near(j)

    def contract_far(j):
        contract(j, 3, 1)
        send_far(j)

    def contract_all(j):
        take(("dt", j), "bundle", 1)
        contract(j, 0, 4)
        send_far(j)
        send_near(j)

    def pass_last(j):
        take(("f", j), "cols", 2)
        last[j, 1, top] = (
            last[j, 1, top].astype(F32) + last_relay[0, j].astype(F32)
        ).astype(BF16)
        push("cols", ("e", j), last.at[j, 1, top], last_in.at[0, j, top], y_up)
        last[j, 2, low] = (
            last[j, 2, low].astype(F32) + last_relay[1, j].astype(F32)
        ).astype(BF16)
        push("cols", ("e", j), last.at[j, 2, low], last_in.at[1, j, low], y_down)

    def finish(j):
        take(("e", j), "cols", 4)
        cols = pl.ds(pl.multiple_of(at_z(spots[j]) * 256, 256), 256)
        total = last[j, 0].astype(F32) + last_in[0, j].astype(F32) + last_in[1, j].astype(F32)
        out_ref[:, cols] = (middle[:, cols] + total).astype(BF16)

    halo()
    own_up.wait()
    z_hop("u", 0)
    own_gate.wait()
    gate_start()
    send_x("u", 0)
    gate_hop(0, 0)
    q_copy.wait()
    attend_early()
    own_down.wait()
    z_hop("d", 0)
    attend_second()
    send_x("d", 0)
    wait_halos()
    attend_third()
    wo_copy.wait()
    z_hop("u", 1)
    send_x("u", 1)
    project(3)
    gate_relay()
    gate_hop(1, 0)
    gate_hop(-1, 0)
    attend_late()
    gate_hop(0, 1)
    project(1)
    relay_x("u", 0)
    project(2)
    project(0)
    send_x("u", 2)
    relay_x("d", 0)
    z_hop("u", 2)
    send_x("u", 3)
    relay_x("u", 1)
    gate_close()
    gate_hop(2, 0)
    gate_twin(0)
    gate_hop(1, 1)
    close_x("u", 0)
    pass_first()
    send_x("u", 4)
    gate_hop(-1, 1)
    relay_x("u", 2)
    close_x("d", 0)
    gate_hop(0, 2)
    relay_x("u", 3)
    z_hop("u", 3)
    send_x("u", 5)
    close_x("u", 1)
    send_x("u", 6)
    gate_hop(2, 1)
    gate_twin(1)
    relay_x("u", 4)
    close_x("u", 2)
    gate_hop(1, 2)
    close_x("u", 3)
    gate_hop(-1, 2)
    norm()
    relay_x("u", 5)
    gate_hop(0, 3)
    relay_x("u", 6)
    z_hop("u", 4)
    send_x("u", 7)
    close_x("u", 4)
    z_hop("d", 1)
    send_x("d", 1)
    close_x("u", 5)
    gate_hop(2, 2)
    gate_twin(2)
    send_x("d", 2)
    close_x("u", 6)
    gate_hop(1, 3)
    relay_x("u", 7)
    gate_hop(-1, 3)
    spread_relay()
    gate_hop(0, 4)
    relay_x("d", 1)
    relay_x("d", 2)
    close_x("u", 7)
    gate_hop(2, 3)
    z_hop("d", 2)
    send_x("d", 3)
    send_x("d", 4)
    gate_twin(3)
    close_x("d", 1)
    gate_hop(1, 4)
    spread_near()
    wait_twins("u")
    expand_up(0, 3, 0, 2)
    gate_hop(-1, 4)
    close_x("d", 2)
    expand_up(0, 3, 2, 2)
    gate_hop(2, 4)
    gate_twin(4)
    expand_up(0, 3, 4, 1, True)
    relay_x("d", 3)
    z_hop("d", 3)
    send_x("d", 5)
    send_x("d", 6)
    wait_twins("g")
    expand_gate(0, 3, 0, 2)
    relay_x("d", 4)
    expand_gate(0, 3, 2, 2)
    spread_far()
    expand_up(3, 1, 0, 5, True)
    z_hop("d", 4)
    send_x("d", 7)
    close_x("d", 3)
    expand_gate(0, 3, 4, 1, True)
    relay_x("d", 5)
    contract_near(0)
    contract_near(1)
    relay_x("d", 6)
    contract_near(2)
    expand_gate(3, 1, 0, 5, True)
    close_x("d", 4)
    contract_far(0)
    relay_x("d", 7)
    contract_far(1)
    contract_far(2)
    close_x("d", 5)
    contract_near(3)
    close_x("d", 6)
    contract_far(3)
    contract_all(4)
    pass_last(0)
    close_x("d", 7)
    contract_all(5)
    pass_last(1)
    pass_last(2)
    contract_all(6)
    contract_all(7)
    pass_last(3)
    pass_last(4)
    finish(0)
    pass_last(5)
    finish(1)
    finish(2)
    pass_last(6)
    pass_last(7)
    finish(3)
    finish(4)
    finish(5)
    finish(6)
    finish(7)
    wait_sent()
    assert (len(sent), len(arriving)) == (N_SENT, N_ARRIVING)


def shards(
    queries,
    key_rows,
    value_rows,
    sink_logits,
    residual,
    norm_gain,
    out_weight,
    gate_weight,
    up_weight,
    down_weight,
):
    tok, width = queries.shape
    d = residual.shape[1]
    rows, ff = gate_weight.shape
    share = tok // 4
    whole = pltpu.VMEM((ZN, XN, CN, rows, ff), BF16)
    narrow = d // LAST_CHUNKS
    hbm = pl.BlockSpec(memory_space=pl.ANY)
    smem = pl.BlockSpec(memory_space=pltpu.SMEM)
    return pl.pallas_call(
        functools.partial(body, tok * lax.axis_size("sp")),
        out_shape=pltpu.VMEM((share, d), BF16),
        in_specs=[hbm, hbm, hbm, smem, hbm, hbm, hbm, hbm, hbm, hbm],
        out_specs=pl.BlockSpec(memory_space=pltpu.VMEM),
        scratch_shapes=[
            pltpu.VMEM((tok, width), BF16),
            pltpu.VMEM((tok + 2 * WIN, DH), BF16),
            pltpu.VMEM((tok + 2 * WIN, DH), BF16),
            pltpu.VMEM((share, d), BF16),
            pltpu.VMEM((1, d), F32),
            pltpu.VMEM((width, d), BF16),
            whole,
            whole,
            whole,
            pltpu.VMEM((tok, width), BF16),
            pltpu.VMEM((4, share, d), BF16),
            pltpu.VMEM((2, share // 2, d), BF16),
            pltpu.VMEM((2, share, d), BF16),
            pltpu.VMEM((share, d), F32),
            pltpu.VMEM((4, share, d), BF16),
            pltpu.VMEM((tok, ff), F32),
            pltpu.VMEM((tok, ff), BF16),
            pltpu.VMEM((LAST_CHUNKS, 4, share, narrow), BF16),
            pltpu.VMEM((2, LAST_CHUNKS, share // 2, narrow), BF16),
            pltpu.VMEM((2, LAST_CHUNKS, share, narrow), BF16),
            pltpu.SemaphoreType.DMA((N_SENT,)),
            pltpu.SemaphoreType.DMA((N_ARRIVING,)),
            pltpu.SemaphoreType.DMA((9,)),
        ],
        compiler_params=pltpu.CompilerParams(
            collective_id=0, has_side_effects=True, vmem_limit_bytes=67043328 - 2**19
        ),
        name="layer",
    )(
        queries,
        key_rows,
        value_rows,
        sink_logits,
        residual,
        norm_gain.reshape(1, d),
        out_weight,
        gate_weight,
        up_weight,
        down_weight.T,
    )


def solution(mesh):
    placed = (
        P("sp", "tp"),
        P("sp", "tp"),
        P("sp", "tp"),
        P("tp"),
        P("sp", None),
        P(),
        P("tp", None),
        P("sp", "tp"),
        P("sp", "tp"),
        P("tp", "sp"),
    )
    return jax.shard_map(
        shards, mesh=mesh, in_specs=placed, out_specs=P(("sp", "tp"), None), check_vma=False
    )
```

```python
import functools

import jax
import jax.numpy as jnp
from jax import lax
from jax.experimental import pallas as pl
from jax.experimental.pallas import tpu as pltpu
from jax.sharding import PartitionSpec as P

DH = 128
WIN = 128
EPSILON = 1e-06
MASKED = -1e30
ZN, XN, CN = 8, 4, 2
MESH = pl.DeviceIdType.MESH
F32 = jnp.float32
BF16 = jnp.bfloat16
N_SENT, N_ARRIVING = 46, 109
LAST_CHUNKS = 8
DIRECT = 7
TAIL = 128


def body(
    seq_len,
    q_hbm,
    k_hbm,
    v_hbm,
    sink_ref,
    res_hbm,
    gain_hbm,
    wo_hbm,
    g_hbm,
    u_hbm,
    d_hbm,
    out_ref,
    q_ref,
    kbuf,
    vbuf,
    res_ref,
    gain_ref,
    wo_ref,
    gate,
    up,
    down,
    att,
    first,
    first_relay,
    first_in,
    middle,
    normed,
    up_acc,
    hidden,
    last,
    last_relay,
    last_in,
    far_in,
    send_sems,
    recv_sems,
    local_sems,
):
    sp = lax.axis_index("sp")
    y = lax.axis_index("tp")
    n_sp = lax.axis_size("sp")
    c = lax.rem(sp, CN)
    x = lax.rem(lax.div(sp, CN), XN)
    z = lax.div(sp, CN * XN)
    tok = q_ref.shape[0]
    share = tok // 4
    half = share // 2
    part = half // 2
    top, low = pl.ds(0, part), pl.ds(part, part)

    def at_z(k):
        return lax.rem(z + (k + ZN), ZN)

    def at_x(k):
        return lax.rem(x + (k + XN), XN)

    def spot(zz, xx, cc):
        return {"sp": (zz * XN + xx) * CN + cc, "tp": y}

    z_up, z_down = spot(at_z(1), x, c), spot(at_z(-1), x, c)
    x_up, x_down = spot(z, at_x(1), c), spot(z, at_x(-1), c)
    twin = spot(z, x, 1 - c)
    y_up = {"sp": sp, "tp": lax.rem(y + 1, 4)}
    y_down = {"sp": sp, "tp": lax.rem(y + 3, 4)}
    y_far = {"sp": sp, "tp": lax.rem(y + 2, 4)}
    right = {"sp": lax.rem(sp + 1, n_sp), "tp": y}
    left = {"sp": lax.rem(sp + n_sp - 1, n_sp), "tp": y}

    lo, hi = pl.ds(0, 16), pl.ds(16, 16)
    sent, arriving = [], {}
    kinds = {
        "halo": (4, lambda n: kbuf.at[pl.ds(0, n * WIN)]),
        "rows": (2, lambda n: first.at[0, 0, pl.ds(0, n * part)]),
        "cols": (8, lambda n: last.at[pl.ds(0, n), 0, 0, top]),
    }

    for name, ref in (("g", gate), ("u", up), ("d", down)):
        kinds["block", name] = (8, lambda n, ref=ref: ref.at[pl.ds(0, n), 0, 0])
        kinds["part", name] = (8, lambda n, ref=ref: ref.at[pl.ds(0, n), 0, 0, lo])
        kinds["bundle", name] = (8, lambda n, ref=ref: ref.at[pl.ds(0, n), :, 0])

    def push(kind, key, src, dst, device):
        groups = [i for i, (of, n) in enumerate(sent) if of == kind and n < kinds[kind][0]]
        if groups:
            i = groups[0]
            sent[i] = (kind, sent[i][1] + 1)
        else:
            i = len(sent)
            sent.append((kind, 1))
        pltpu.make_async_remote_copy(
            src_ref=src,
            dst_ref=dst,
            send_sem=send_sems.at[i],
            recv_sem=recv_sems.at[arriving.setdefault(key, len(arriving))],
            device_id=device,
            device_id_type=MESH,
        ).start()

    def wait_bytes(sem, ref):
        pltpu.make_async_copy(ref, ref, sem).wait()

    def take(key, kind, n):
        wait_bytes(recv_sems.at[arriving[key]], kinds[kind][1](n))

    def wait_sent():
        for i, (kind, n) in enumerate(sent):
            wait_bytes(send_sems.at[i], kinds[kind][1](n))

    def local(i, src, dst):
        copy = pltpu.make_async_copy(src, dst, local_sems.at[i])
        copy.start()
        return copy

    k_copy = local(0, k_hbm, kbuf.at[pl.ds(WIN, tok)])
    v_copy = local(1, v_hbm, vbuf.at[pl.ds(WIN, tok)])
    ff, cut = u_hbm.shape[1], gate.shape[4]
    own_up = (
        local(2, u_hbm, up.at[z, x, c, :, pl.ds(0, ff)]),
        local(9, g_hbm.at[:, pl.ds(cut, TAIL)], up.at[z, x, c, :, pl.ds(ff, TAIL)]),
    )
    own_gate = local(3, g_hbm.at[:, pl.ds(0, cut)], gate.at[z, x, c])
    own_down = local(4, d_hbm, down.at[z, x, c])
    q_copy = local(5, q_hbm, q_ref)
    wo_copy = local(6, wo_hbm, wo_ref)
    res_copy = local(7, res_hbm.at[pl.ds(pl.multiple_of(y * share, share), share)], res_ref)
    gain_copy = local(8, gain_hbm, gain_ref)

    barrier = pltpu.get_barrier_semaphore()
    peers = (x_up, x_down, z_up, z_down, twin, y_up, y_down, y_far, left, right)
    for peer in peers:
        pl.semaphore_signal(barrier, inc=1, device_id=peer, device_id_type=MESH)
    pl.semaphore_wait(barrier, len(peers))

    buffers = {"u": up, "d": down}
    spots = (0, -1, 1, -2, 2, -3, 3, 4)

    def halo():
        k_copy.wait()
        v_copy.wait()
        for start, to, device in ((tok, 0, right), (WIN, WIN + tok, left)):
            for ref in (kbuf, vbuf):
                push("halo", "halo", ref.at[pl.ds(start, WIN)], ref.at[pl.ds(to, WIN)], device)

    def wait_halos():
        take("halo", "halo", 4)

    def to_twin(m, key, ref):
        push(("bundle", m), key, ref, ref, twin)

    def hop(m, flow, k, block, halves):
        if k:
            take((flow, k), ("block", m), 2 if k < 4 else 1)
        if k < 4:
            for way, zz, to in ((0, at_z(-k), z_up), (1, at_z(k), z_down)):
                ref = block(zz)
                if k == 3:
                    ref = ref.at[halves[way]]
                push(("block" if k < 3 else "part", m), (flow, k + 1), ref, ref, to)

    def z_hop(m, k):
        hop(m, m, k, lambda zz: buffers[m].at[zz, x, c], (lo, hi))

    def gate_hop(i, k):
        hop("g", i, k, lambda zz: gate.at[zz, at_x(i), c], (lo, hi))

    def gate_twin(k):
        for kk in sorted({-k, k if k < 4 else -k}):
            to_twin("g", "gt", gate.at[at_z(kk), :, c])

    def along_x(m, key, block):
        push(("block", m), key, block, block, x_up)
        push(("block", m), key, block, block, x_down)

    def relay_along_x(m, key, later, line):
        take(key, ("block", m), 2)
        for piece, to in ((line.at[at_x(-1), c, lo], x_up), (line.at[at_x(1), c, hi], x_down)):
            push(("part", m), later, piece, piece, to)

    def send_x(m, j):
        along_x(m, ("x", m, j), buffers[m].at[at_z(spots[j]), x, c])

    def relay_x(m, j):
        relay_along_x(m, ("x", m, j), ("r", m, j), buffers[m].at[at_z(spots[j])])

    def close_x(m, j):
        take(("r", m, j), ("block", m), 1)
        to_twin(m, "ut" if m == "u" else ("dt", j), buffers[m].at[at_z(spots[j]), :, c])

    def gate_start():
        along_x("g", "gx", gate.at[z, x, c])

    def gate_relay():
        relay_along_x("g", "gx", "gr", gate.at[z])

    def gate_close():
        take("gr", ("block", "g"), 1)

    def wait_twins(m):
        take(m + "t", ("bundle", m), 8)

    offset = sp * tok
    shares = {0: y, 1: lax.rem(y + 1, 4), 2: lax.rem(y + 3, 4), 3: lax.rem(y + 2, 4)}
    late = lax.div(y, 2)
    inner = lax.rem(lax.div(y + 1, 2), 2)

    def attend(b):
        start = pl.multiple_of(b * share, share)
        span = share + 2 * WIN
        keys = kbuf[pl.ds(start, span), :]
        values = vbuf[pl.ds(start, span), :]
        row = lax.broadcasted_iota(jnp.int32, (share, span), 0)
        col = lax.broadcasted_iota(jnp.int32, (share, span), 1)
        gap = col - row
        place = col + (offset + start - WIN)
        kept = (gap >= 0) & (gap <= 2 * WIN) & (place >= 0) & (place < seq_len)
        for h in range(q_ref.shape[1] // DH):
            query = q_ref[pl.ds(start, share), pl.ds(h * DH, DH)]
            score = lax.dot_general(
                query, keys, (((1,), (1,)), ((), ())), preferred_element_type=F32
            ) * DH ** (-0.5)
            score = jnp.where(kept, score, MASKED)
            sink = sink_ref[h]
            most = jnp.maximum(jnp.max(score, axis=-1, keepdims=True), sink)
            weight = jnp.exp(score - most)
            total = jnp.sum(weight, axis=-1, keepdims=True) + jnp.exp(sink - most)
            prob = (weight * (1.0 / total)).astype(BF16)
            att[pl.ds(start, share), pl.ds(h * DH, DH)] = jnp.dot(
                prob, values, preferred_element_type=F32
            ).astype(BF16)

    def attend_early():
        attend(lax.rem(y + 1 + 2 * late, 4))

    def attend_second():
        attend(lax.rem(y + 2 * (1 - inner), 4))

    def attend_third():
        attend(lax.rem(y + 2 * inner, 4))

    def attend_late():
        attend(lax.rem(y + 3 + 2 * late, 4))

    def project(place):
        start = pl.multiple_of(shares[place] * share, share)
        product = jnp.dot(
            att[pl.ds(start, share), :], wo_ref[...], preferred_element_type=F32
        ).astype(BF16)
        for g in range(2):
            first[g, place] = product[g * half : (g + 1) * half]
        for g in range(2):
            if place == 3:
                push("rows", ("far", g), first.at[g, 3, top], first_relay.at[g, 0], y_up)
                push("rows", ("far", g), first.at[g, 3, low], first_relay.at[g, 1], y_down)

    def first_near(g):
        push("rows", ("near", g), first.at[g, 1, low], first_in.at[g, 0, low], y_up)
        push("rows", ("near", g), first.at[g, 2, top], first_in.at[g, 1, top], y_down)

    def pass_first(g):
        take(("far", g), "rows", 2)
        first[g, 1, top] = (
            first[g, 1, top].astype(F32) + first_relay[g, 0].astype(F32)
        ).astype(BF16)
        push("rows", ("near", g), first.at[g, 1, top], first_in.at[g, 0, top], y_up)
        first[g, 2, low] = (
            first[g, 2, low].astype(F32) + first_relay[g, 1].astype(F32)
        ).astype(BF16)
        push("rows", ("near", g), first.at[g, 2, low], first_in.at[g, 1, low], y_down)

    rows_in = middle.shape[2]

    def norm(g):
        if g == 0:
            res_copy.wait()
            gain_copy.wait()
        wait_bytes(recv_sems.at[arriving["near", g]], first.at[g, pl.ds(0, 2)])
        squares = jnp.zeros((half, 1), F32)
        width = 512
        for n in range(rows_in // width):
            cols = pl.ds(n * width, width)
            rows = res_ref[pl.ds(g * half, half), cols].astype(F32) + (
                first[g, 0, :, cols].astype(F32)
                + first_in[g, 0, :, cols].astype(F32)
                + first_in[g, 1, :, cols].astype(F32)
            )
            middle[g, :, cols] = rows
            squares += jnp.sum(rows * rows, axis=-1, keepdims=True)
        scale = lax.rsqrt(squares * (1.0 / rows_in) + EPSILON)
        for n in range(rows_in // width):
            cols = pl.ds(n * width, width)
            normed[g, 0, :, cols] = (middle[g, :, cols] * scale * gain_ref[:, cols]).astype(BF16)
        push("rows", ("s0", g), normed.at[g, 0, top], normed.at[g, 2, top], y_up)
        push("rows", ("s0", g), normed.at[g, 0, low], normed.at[g, 1, low], y_down)
        push("rows", ("s1", g), normed.at[g, 0, low], normed.at[g, 2, low], y_up)
        push("rows", ("s1", g), normed.at[g, 0, top], normed.at[g, 1, top], y_down)

    def spread_relay(g):
        take(("s0", g), "rows", 2)
        push("rows", ("s2", g), normed.at[g, 2, top], normed.at[g, 3, top], y_up)
        push("rows", ("s2", g), normed.at[g, 1, low], normed.at[g, 3, low], y_down)

    def spread_end(g):
        take(("s1", g), "rows", 2)
        take(("s2", g), "rows", 2)

    def over_tiles(tile, first_tile, tiles):
        def step(t, carry):
            tile(pl.ds(pl.multiple_of(t * 256, 256), 256))
            return carry

        lax.fori_loop(first_tile, first_tile + tiles, step, 0)

    def times(weight, g, cols):
        return jnp.dot(
            normed[g].reshape(tok // 2, rows_in),
            weight[:, :, :, :, cols].reshape(rows_in, cols.size),
            preferred_element_type=F32,
        )

    def expand_up(g, first_tile, tiles):
        def tile(cols):
            up_acc[g, :, cols] = times(up, g, cols)

        over_tiles(tile, first_tile, tiles)

    def open_gate(g, cols, g_acc, u_acc):
        hidden[g, :, cols] = (g_acc / (1.0 + jnp.exp(-g_acc)) * u_acc).astype(BF16)

    def expand_tail(g):
        both = times(up, g, pl.ds(cut, 2 * TAIL))
        open_gate(g, pl.ds(cut, TAIL), both[:, TAIL:], both[:, :TAIL])

    def expand_gate(g, first_tile, tiles):
        def tile(cols):
            open_gate(g, cols, times(gate, g, cols), up_acc[g, :, cols])

        over_tiles(tile, first_tile, tiles)

    def contract(j, g):
        if g == 0:
            take(("dt", j), ("bundle", "d"), 1)
        product = lax.dot_general(
            hidden[g],
            down[at_z(spots[j])].reshape(256, hidden.shape[2]),
            (((1,), (1,)), ((), ())),
            preferred_element_type=F32,
        )
        last[j, g] = product.astype(BF16).reshape(4, half, 256)
        if j >= DIRECT:
            for rows in (top, low):
                push("cols", ("e", j, g), last.at[j, g, 3, rows], far_in.at[j - DIRECT, g, rows], y_far)
                push("cols", ("e", j, g), last.at[j, g, 1, rows], last_in.at[j, g, 0, rows], y_up)
                push("cols", ("e", j, g), last.at[j, g, 2, rows], last_in.at[j, g, 1, rows], y_down)
            return
        push("cols", ("f", j, g), last.at[j, g, 3, top], last_relay.at[j, g, 0], y_up)
        push("cols", ("f", j, g), last.at[j, g, 3, low], last_relay.at[j, g, 1], y_down)
        push("cols", ("e", j, g), last.at[j, g, 1, low], last_in.at[j, g, 0, low], y_up)
        push("cols", ("e", j, g), last.at[j, g, 2, top], last_in.at[j, g, 1, top], y_down)

    def pass_last(j, g):
        take(("f", j, g), "cols", 2)
        last[j, g, 1, top] = (
            last[j, g, 1, top].astype(F32) + last_relay[j, g, 0].astype(F32)
        ).astype(BF16)
        push("cols", ("e", j, g), last.at[j, g, 1, top], last_in.at[j, g, 0, top], y_up)
        last[j, g, 2, low] = (
            last[j, g, 2, low].astype(F32) + last_relay[j, g, 1].astype(F32)
        ).astype(BF16)
        push("cols", ("e", j, g), last.at[j, g, 2, low], last_in.at[j, g, 1, low], y_down)

    def finish(j, g):
        take(("e", j, g), "cols", 6 if j >= DIRECT else 4)
        cols = pl.ds(pl.multiple_of(at_z(spots[j]) * 256, 256), 256)
        total = (
            last[j, g, 0].astype(F32)
            + last_in[j, g, 0].astype(F32)
            + last_in[j, g, 1].astype(F32)
        )
        if j >= DIRECT:
            total += far_in[j - DIRECT, g].astype(F32)
        out_ref[pl.ds(g * half, half), cols] = (middle[g, :, cols] + total).astype(BF16)

    halo()
    for copy in own_up:
        copy.wait()
    z_hop("u", 0)
    own_gate.wait()
    gate_start()
    send_x("u", 0)
    gate_hop(0, 0)
    q_copy.wait()
    attend_early()
    attend_second()
    own_down.wait()
    z_hop("d", 0)
    wait_halos()
    attend_third()
    wo_copy.wait()
    z_hop("u", 1)
    send_x("u", 1)
    send_x("u", 2)
    project(3)
    gate_relay()
    attend_late()
    gate_hop(1, 0)
    project(1)
    relay_x("u", 0)
    gate_hop(-1, 0)
    project(2)
    first_near(0)
    project(0)
    gate_hop(0, 1)
    relay_x("u", 1)
    z_hop("u", 2)
    send_x("u", 3)
    send_x("u", 4)
    relay_x("u", 2)
    gate_close()
    gate_hop(2, 0)
    gate_twin(0)
    pass_first(0)
    first_near(1)
    close_x("u", 0)
    pass_first(1)
    gate_hop(1, 1)
    close_x("u", 1)
    gate_hop(-1, 1)
    relay_x("u", 3)
    z_hop("u", 3)
    send_x("u", 5)
    send_x("u", 6)
    relay_x("u", 4)
    norm(0)
    gate_hop(0, 2)
    close_x("u", 2)
    close_x("u", 3)
    gate_hop(2, 1)
    gate_twin(1)
    gate_hop(1, 2)
    relay_x("u", 5)
    z_hop("u", 4)
    send_x("u", 7)
    gate_hop(-1, 2)
    relay_x("u", 6)
    close_x("u", 4)
    gate_hop(0, 3)
    close_x("u", 5)
    send_x("d", 0)
    spread_relay(0)
    norm(1)
    gate_hop(2, 2)
    gate_twin(2)
    z_hop("d", 1)
    send_x("d", 1)
    relay_x("u", 7)
    close_x("u", 6)
    gate_hop(1, 3)
    gate_hop(-1, 3)
    gate_hop(0, 4)
    send_x("d", 2)
    relay_x("d", 0)
    spread_end(0)
    gate_hop(2, 3)
    gate_twin(3)
    relay_x("d", 1)
    close_x("u", 7)
    z_hop("d", 2)
    spread_relay(1)
    send_x("d", 3)
    gate_hop(1, 4)
    relay_x("d", 2)
    gate_hop(-1, 4)
    wait_twins("u")
    expand_up(0, 0, 3)
    gate_hop(2, 4)
    gate_twin(4)
    close_x("d", 0)
    expand_up(0, 3, 2)
    expand_tail(0)
    send_x("d", 4)
    close_x("d", 1)
    z_hop("d", 3)
    wait_twins("g")
    expand_gate(0, 0, 2)
    spread_end(1)
    relay_x("d", 3)
    expand_gate(0, 2, 3)
    send_x("d", 5)
    close_x("d", 2)
    contract(0, 0)
    contract(1, 0)
    z_hop("d", 4)
    expand_up(1, 0, 3)
    relay_x("d", 4)
    contract(2, 0)
    send_x("d", 6)
    close_x("d", 3)
    expand_up(1, 3, 2)
    expand_tail(1)
    pass_last(0, 0)
    expand_gate(1, 0, 2)
    pass_last(1, 0)
    relay_x("d", 5)
    expand_gate(1, 2, 3)
    pass_last(2, 0)
    send_x("d", 7)
    close_x("d", 4)
    contract(3, 0)
    contract(0, 1)
    contract(1, 1)
    relay_x("d", 6)
    contract(2, 1)
    contract(4, 0)
    close_x("d", 5)
    contract(3, 1)
    pass_last(3, 0)
    contract(4, 1)
    pass_last(0, 1)
    finish(0, 0)
    finish(1, 0)
    finish(2, 0)
    relay_x("d", 7)
    pass_last(1, 1)
    contract(5, 0)
    pass_last(2, 1)
    close_x("d", 6)
    contract(5, 1)
    pass_last(4, 0)
    pass_last(3, 1)
    finish(3, 0)
    pass_last(4, 1)
    close_x("d", 7)
    contract(6, 0)
    contract(6, 1)
    pass_last(5, 0)
    finish(0, 1)
    finish(1, 1)
    finish(2, 1)
    contract(7, 0)
    pass_last(5, 1)
    contract(7, 1)
    finish(4, 0)
    finish(3, 1)
    finish(4, 1)
    pass_last(6, 0)
    pass_last(6, 1)
    finish(5, 0)
    finish(7, 0)
    finish(5, 1)
    finish(7, 1)
    finish(6, 0)
    finish(6, 1)
    wait_sent()
    assert (len(sent), len(arriving)) == (N_SENT, N_ARRIVING)


def shards(
    queries,
    key_rows,
    value_rows,
    sink_logits,
    residual,
    norm_gain,
    out_weight,
    gate_weight,
    up_weight,
    down_weight,
):
    tok, width = queries.shape
    d = residual.shape[1]
    rows, ff = gate_weight.shape
    share = tok // 4
    half = share // 2
    gate_part, up_part, down_part = (
        pltpu.VMEM((ZN, XN, CN, rows, columns), BF16) for columns in (ff - TAIL, ff + TAIL, ff)
    )
    narrow = d // LAST_CHUNKS
    hbm = pl.BlockSpec(memory_space=pl.ANY)
    smem = pl.BlockSpec(memory_space=pltpu.SMEM)
    return pl.pallas_call(
        functools.partial(body, tok * lax.axis_size("sp")),
        out_shape=pltpu.VMEM((share, d), BF16),
        in_specs=[hbm, hbm, hbm, smem, hbm, hbm, hbm, hbm, hbm, hbm],
        out_specs=pl.BlockSpec(memory_space=pltpu.VMEM),
        scratch_shapes=[
            pltpu.VMEM((tok, width), BF16),
            pltpu.VMEM((tok + 2 * WIN, DH), BF16),
            pltpu.VMEM((tok + 2 * WIN, DH), BF16),
            pltpu.VMEM((share, d), BF16),
            pltpu.VMEM((1, d), F32),
            pltpu.VMEM((width, d), BF16),
            gate_part,
            up_part,
            down_part,
            pltpu.VMEM((tok, width), BF16),
            pltpu.VMEM((2, 4, half, d), BF16),
            pltpu.VMEM((2, 2, half // 2, d), BF16),
            pltpu.VMEM((2, 2, half, d), BF16),
            pltpu.VMEM((2, half, d), F32),
            pltpu.VMEM((2, 4, half, d), BF16),
            pltpu.VMEM((2, tok // 2, ff - TAIL), F32),
            pltpu.VMEM((2, tok // 2, ff), BF16),
            pltpu.VMEM((LAST_CHUNKS, 2, 4, half, narrow), BF16),
            pltpu.VMEM((LAST_CHUNKS, 2, 2, half // 2, narrow), BF16),
            pltpu.VMEM((LAST_CHUNKS, 2, 2, half, narrow), BF16),
            pltpu.VMEM((LAST_CHUNKS - DIRECT, 2, half, narrow), BF16),
            pltpu.SemaphoreType.DMA((N_SENT,)),
            pltpu.SemaphoreType.DMA((N_ARRIVING,)),
            pltpu.SemaphoreType.DMA((10,)),
        ],
        compiler_params=pltpu.CompilerParams(
            collective_id=0, has_side_effects=True, vmem_limit_bytes=67043328 - 2**19
        ),
        name="layer",
    )(
        queries,
        key_rows,
        value_rows,
        sink_logits,
        residual,
        norm_gain.reshape(1, d),
        out_weight,
        gate_weight,
        up_weight,
        down_weight.T,
    )


def solution(mesh):
    placed = (
        P("sp", "tp"),
        P("sp", "tp"),
        P("sp", "tp"),
        P("tp"),
        P("sp", None),
        P(),
        P("tp", None),
        P("sp", "tp"),
        P("sp", "tp"),
        P("tp", "sp"),
    )
    return jax.shard_map(
        shards, mesh=mesh, in_specs=placed, out_specs=P(("sp", "tp"), None), check_vma=False
    )
```

```python
import functools

import jax
import jax.numpy as jnp
from jax import lax
from jax.experimental import pallas as pl
from jax.experimental.pallas import tpu as pltpu
from jax.sharding import PartitionSpec as P

DH = 128
WIN = 128
EPSILON = 1e-06
MASKED = -1e30
ZN, XN, CN = 8, 4, 2
MESH = pl.DeviceIdType.MESH
F32 = jnp.float32
BF16 = jnp.bfloat16
N_SENT, N_ARRIVING = 48, 109
LAST_CHUNKS = 8
DIRECT = 7
PIECES = 5
TAIL = 128


def body(
    seq_len,
    q_hbm,
    k_hbm,
    v_hbm,
    sink_ref,
    res_hbm,
    gain_hbm,
    wo_hbm,
    g_hbm,
    u_hbm,
    d_hbm,
    out_ref,
    q_ref,
    kbuf,
    vbuf,
    res_ref,
    gain_ref,
    wo_ref,
    gate,
    up,
    down,
    att,
    first,
    first_relay,
    first_in,
    middle,
    normed,
    up_acc,
    hidden,
    last,
    last_relay,
    last_in,
    far_in,
    send_sems,
    recv_sems,
    local_sems,
):
    sp = lax.axis_index("sp")
    y = lax.axis_index("tp")
    n_sp = lax.axis_size("sp")
    c = lax.rem(sp, CN)
    x = lax.rem(lax.div(sp, CN), XN)
    z = lax.div(sp, CN * XN)
    tok = q_ref.shape[0]
    share = tok // 4
    half = share // 2
    part = half // 2
    top, low = pl.ds(0, part), pl.ds(part, part)

    def at_z(k):
        return lax.rem(z + (k + ZN), ZN)

    def at_x(k):
        return lax.rem(x + (k + XN), XN)

    def spot(zz, xx, cc):
        return {"sp": (zz * XN + xx) * CN + cc, "tp": y}

    z_up, z_down = spot(at_z(1), x, c), spot(at_z(-1), x, c)
    x_up, x_down = spot(z, at_x(1), c), spot(z, at_x(-1), c)
    twin = spot(z, x, 1 - c)
    y_up = {"sp": sp, "tp": lax.rem(y + 1, 4)}
    y_down = {"sp": sp, "tp": lax.rem(y + 3, 4)}
    y_far = {"sp": sp, "tp": lax.rem(y + 2, 4)}
    right = {"sp": lax.rem(sp + 1, n_sp), "tp": y}
    left = {"sp": lax.rem(sp + n_sp - 1, n_sp), "tp": y}

    lo, hi = pl.ds(0, 16), pl.ds(16, 16)
    sent, arriving = [], {}
    kinds = {
        "halo": (4, lambda n: kbuf.at[pl.ds(0, n * WIN)]),
        "rows": (2, lambda n: first.at[0, 0, pl.ds(0, n * part)]),
        "cols": (8, lambda n: last.at[pl.ds(0, n), 0, 0, top]),
    }

    for name, ref in (("g", gate), ("u", up), ("d", down)):
        kinds["block", name] = (8, lambda n, ref=ref: ref.at[pl.ds(0, n), 0, 0])
        kinds["part", name] = (8, lambda n, ref=ref: ref.at[pl.ds(0, n), 0, 0, lo])
        kinds["bundle", name] = (8, lambda n, ref=ref: ref.at[pl.ds(0, n), :, 0])

    def push(kind, key, src, dst, device):
        groups = [i for i, (of, n) in enumerate(sent) if of == kind and n < kinds[kind][0]]
        if groups:
            i = groups[0]
            sent[i] = (kind, sent[i][1] + 1)
        else:
            i = len(sent)
            sent.append((kind, 1))
        pltpu.make_async_remote_copy(
            src_ref=src,
            dst_ref=dst,
            send_sem=send_sems.at[i],
            recv_sem=recv_sems.at[arriving.setdefault(key, len(arriving))],
            device_id=device,
            device_id_type=MESH,
        ).start()

    def wait_bytes(sem, ref):
        pltpu.make_async_copy(ref, ref, sem).wait()

    def take(key, kind, n):
        wait_bytes(recv_sems.at[arriving[key]], kinds[kind][1](n))

    def wait_sent():
        for i, (kind, n) in enumerate(sent):
            wait_bytes(send_sems.at[i], kinds[kind][1](n))

    def local(i, src, dst):
        copy = pltpu.make_async_copy(src, dst, local_sems.at[i])
        copy.start()
        return copy

    k_copy = local(0, k_hbm, kbuf.at[pl.ds(WIN, tok)])
    v_copy = local(1, v_hbm, vbuf.at[pl.ds(WIN, tok)])
    ff, cut = u_hbm.shape[1], gate.shape[4]
    own_up = (
        local(2, u_hbm, up.at[z, x, c, :, pl.ds(0, ff)]),
        local(9, g_hbm.at[:, pl.ds(cut, TAIL)], up.at[z, x, c, :, pl.ds(ff, TAIL)]),
    )
    own_gate = local(3, g_hbm.at[:, pl.ds(0, cut)], gate.at[z, x, c])
    own_down = local(4, d_hbm, down.at[z, x, c])
    q_copy = local(5, q_hbm, q_ref)
    wo_copy = local(6, wo_hbm, wo_ref)
    res_copy = local(7, res_hbm.at[pl.ds(pl.multiple_of(y * share, share), share)], res_ref)
    gain_copy = local(8, gain_hbm, gain_ref)

    barrier = pltpu.get_barrier_semaphore()
    peers = (x_up, x_down, z_up, z_down, twin, y_up, y_down, y_far, left, right)
    for peer in peers:
        pl.semaphore_signal(barrier, inc=1, device_id=peer, device_id_type=MESH)
    pl.semaphore_wait(barrier, len(peers))

    buffers = {"u": up, "d": down}
    spots = (0, -1, 1, -2, 2, -3, 3, 4)

    def halo():
        k_copy.wait()
        v_copy.wait()
        for start, to, device in ((tok, 0, right), (WIN, WIN + tok, left)):
            for ref in (kbuf, vbuf):
                push("halo", "halo", ref.at[pl.ds(start, WIN)], ref.at[pl.ds(to, WIN)], device)

    def wait_halos():
        take("halo", "halo", 4)

    def to_twin(m, key, ref):
        push(("bundle", m), key, ref, ref, twin)

    def hop(m, flow, k, block, halves):
        if k:
            take((flow, k), ("block", m), 2 if k < 4 else 1)
        if k < 4:
            for way, zz, to in ((0, at_z(-k), z_up), (1, at_z(k), z_down)):
                ref = block(zz)
                if k == 3:
                    ref = ref.at[halves[way]]
                push(("block" if k < 3 else "part", m), (flow, k + 1), ref, ref, to)

    def z_hop(m, k):
        hop(m, m, k, lambda zz: buffers[m].at[zz, x, c], (lo, hi))

    def gate_hop(i, k):
        hop("g", i, k, lambda zz: gate.at[zz, at_x(i), c], (lo, hi))

    def gate_twin(k):
        for kk in sorted({-k, k if k < 4 else -k}):
            to_twin("g", "gt", gate.at[at_z(kk), :, c])

    def along_x(m, key, block):
        push(("block", m), key, block, block, x_up)
        push(("block", m), key, block, block, x_down)

    def relay_along_x(m, key, later, line):
        take(key, ("block", m), 2)
        for piece, to in ((line.at[at_x(-1), c, lo], x_up), (line.at[at_x(1), c, hi], x_down)):
            push(("part", m), later, piece, piece, to)

    def send_x(m, j):
        along_x(m, ("x", m, j), buffers[m].at[at_z(spots[j]), x, c])

    def relay_x(m, j):
        line = buffers[m].at[at_z(spots[j])]
        relay_along_x(m, ("x", m, j), ("r", m, j), line)
        if m == "d" and j >= PIECES:
            for k in (0, -1, 1):
                block = line.at[at_x(k), c]
                push(("block", m), ("dt", j), block, block, twin)

    def close_x(m, j):
        take(("r", m, j), ("block", m), 1)
        if m == "d" and j >= PIECES:
            block = buffers[m].at[at_z(spots[j]), at_x(2), c]
            push(("block", m), ("dt", j), block, block, twin)
            return
        to_twin(m, "ut" if m == "u" else ("dt", j), buffers[m].at[at_z(spots[j]), :, c])

    def gate_start():
        along_x("g", "gx", gate.at[z, x, c])

    def gate_relay():
        relay_along_x("g", "gx", "gr", gate.at[z])

    def gate_close():
        take("gr", ("block", "g"), 1)

    def wait_twins(m):
        take(m + "t", ("bundle", m), 8)

    offset = sp * tok
    shares = {0: y, 1: lax.rem(y + 1, 4), 2: lax.rem(y + 3, 4), 3: lax.rem(y + 2, 4)}
    late = lax.div(y, 2)
    inner = lax.rem(lax.div(y + 1, 2), 2)

    def attend(b):
        start = pl.multiple_of(b * share, share)
        span = share + 2 * WIN
        keys = kbuf[pl.ds(start, span), :]
        values = vbuf[pl.ds(start, span), :]
        row = lax.broadcasted_iota(jnp.int32, (share, span), 0)
        col = lax.broadcasted_iota(jnp.int32, (share, span), 1)
        gap = col - row
        place = col + (offset + start - WIN)
        kept = (gap >= 0) & (gap <= 2 * WIN) & (place >= 0) & (place < seq_len)
        for h in range(q_ref.shape[1] // DH):
            query = q_ref[pl.ds(start, share), pl.ds(h * DH, DH)]
            score = lax.dot_general(
                query, keys, (((1,), (1,)), ((), ())), preferred_element_type=F32
            ) * DH ** (-0.5)
            score = jnp.where(kept, score, MASKED)
            sink = sink_ref[h]
            most = jnp.maximum(jnp.max(score, axis=-1, keepdims=True), sink)
            weight = jnp.exp(score - most)
            total = jnp.sum(weight, axis=-1, keepdims=True) + jnp.exp(sink - most)
            prob = (weight * (1.0 / total)).astype(BF16)
            att[pl.ds(start, share), pl.ds(h * DH, DH)] = jnp.dot(
                prob, values, preferred_element_type=F32
            ).astype(BF16)

    def attend_early():
        attend(lax.rem(y + 1 + 2 * late, 4))

    def attend_second():
        attend(lax.rem(y + 2 * (1 - inner), 4))

    def attend_third():
        attend(lax.rem(y + 2 * inner, 4))

    def attend_late():
        attend(lax.rem(y + 3 + 2 * late, 4))

    def project(place):
        start = pl.multiple_of(shares[place] * share, share)
        product = jnp.dot(
            att[pl.ds(start, share), :], wo_ref[...], preferred_element_type=F32
        ).astype(BF16)
        for g in range(2):
            first[g, place] = product[g * half : (g + 1) * half]
        for g in range(2):
            if place == 3:
                push("rows", ("far", g), first.at[g, 3, top], first_relay.at[g, 0], y_up)
                push("rows", ("far", g), first.at[g, 3, low], first_relay.at[g, 1], y_down)

    def first_near(g):
        push("rows", ("near", g), first.at[g, 1, low], first_in.at[g, 0, low], y_up)
        push("rows", ("near", g), first.at[g, 2, top], first_in.at[g, 1, top], y_down)

    def pass_first(g):
        take(("far", g), "rows", 2)
        first[g, 1, top] = (
            first[g, 1, top].astype(F32) + first_relay[g, 0].astype(F32)
        ).astype(BF16)
        push("rows", ("near", g), first.at[g, 1, top], first_in.at[g, 0, top], y_up)
        first[g, 2, low] = (
            first[g, 2, low].astype(F32) + first_relay[g, 1].astype(F32)
        ).astype(BF16)
        push("rows", ("near", g), first.at[g, 2, low], first_in.at[g, 1, low], y_down)

    rows_in = middle.shape[2]

    def norm(g):
        if g == 0:
            res_copy.wait()
            gain_copy.wait()
        wait_bytes(recv_sems.at[arriving["near", g]], first.at[g, pl.ds(0, 2)])
        squares = jnp.zeros((half, 1), F32)
        width = 512
        for n in range(rows_in // width):
            cols = pl.ds(n * width, width)
            rows = res_ref[pl.ds(g * half, half), cols].astype(F32) + (
                first[g, 0, :, cols].astype(F32)
                + first_in[g, 0, :, cols].astype(F32)
                + first_in[g, 1, :, cols].astype(F32)
            )
            middle[g, :, cols] = rows
            squares += jnp.sum(rows * rows, axis=-1, keepdims=True)
        scale = lax.rsqrt(squares * (1.0 / rows_in) + EPSILON)
        for n in range(rows_in // width):
            cols = pl.ds(n * width, width)
            normed[g, 0, :, cols] = (middle[g, :, cols] * scale * gain_ref[:, cols]).astype(BF16)
        push("rows", ("s0", g), normed.at[g, 0, top], normed.at[g, 2, top], y_up)
        push("rows", ("s0", g), normed.at[g, 0, low], normed.at[g, 1, low], y_down)
        push("rows", ("s1", g), normed.at[g, 0, low], normed.at[g, 2, low], y_up)
        push("rows", ("s1", g), normed.at[g, 0, top], normed.at[g, 1, top], y_down)

    def spread_relay(g):
        take(("s0", g), "rows", 2)
        push("rows", ("s2", g), normed.at[g, 2, top], normed.at[g, 3, top], y_up)
        push("rows", ("s2", g), normed.at[g, 1, low], normed.at[g, 3, low], y_down)

    def spread_end(g):
        take(("s1", g), "rows", 2)
        take(("s2", g), "rows", 2)

    def over_tiles(tile, first_tile, tiles):
        def step(t, carry):
            tile(pl.ds(pl.multiple_of(t * 256, 256), 256))
            return carry

        lax.fori_loop(first_tile, first_tile + tiles, step, 0)

    def times(weight, g, cols):
        return jnp.dot(
            normed[g].reshape(tok // 2, rows_in),
            weight[:, :, :, :, cols].reshape(rows_in, cols.size),
            preferred_element_type=F32,
        )

    def expand_up(g, first_tile, tiles):
        def tile(cols):
            up_acc[g, :, cols] = times(up, g, cols)

        over_tiles(tile, first_tile, tiles)

    def open_gate(g, cols, g_acc, u_acc):
        hidden[g, :, cols] = (g_acc / (1.0 + jnp.exp(-g_acc)) * u_acc).astype(BF16)

    def expand_tail(g):
        both = times(up, g, pl.ds(cut, 2 * TAIL))
        open_gate(g, pl.ds(cut, TAIL), both[:, TAIL:], both[:, :TAIL])

    def expand_gate(g, first_tile, tiles):
        def tile(cols):
            open_gate(g, cols, times(gate, g, cols), up_acc[g, :, cols])

        over_tiles(tile, first_tile, tiles)

    def contract(j, g):
        if g == 0:
            take(("dt", j), ("bundle", "d"), 1)
        product = lax.dot_general(
            hidden[g],
            down[at_z(spots[j])].reshape(256, hidden.shape[2]),
            (((1,), (1,)), ((), ())),
            preferred_element_type=F32,
        )
        last[j, g] = product.astype(BF16).reshape(4, half, 256)
        if j >= DIRECT:
            for rows in (top, low):
                push("cols", ("e", j, g), last.at[j, g, 3, rows], far_in.at[j - DIRECT, g, rows], y_far)
                push("cols", ("e", j, g), last.at[j, g, 1, rows], last_in.at[j, g, 0, rows], y_up)
                push("cols", ("e", j, g), last.at[j, g, 2, rows], last_in.at[j, g, 1, rows], y_down)
            return
        push("cols", ("f", j, g), last.at[j, g, 3, top], last_relay.at[j, g, 0], y_up)
        push("cols", ("f", j, g), last.at[j, g, 3, low], last_relay.at[j, g, 1], y_down)
        push("cols", ("e", j, g), last.at[j, g, 1, low], last_in.at[j, g, 0, low], y_up)
        push("cols", ("e", j, g), last.at[j, g, 2, top], last_in.at[j, g, 1, top], y_down)

    def pass_last(j, g):
        take(("f", j, g), "cols", 2)
        last[j, g, 1, top] = (
            last[j, g, 1, top].astype(F32) + last_relay[j, g, 0].astype(F32)
        ).astype(BF16)
        push("cols", ("e", j, g), last.at[j, g, 1, top], last_in.at[j, g, 0, top], y_up)
        last[j, g, 2, low] = (
            last[j, g, 2, low].astype(F32) + last_relay[j, g, 1].astype(F32)
        ).astype(BF16)
        push("cols", ("e", j, g), last.at[j, g, 2, low], last_in.at[j, g, 1, low], y_down)

    def finish(j, g):
        take(("e", j, g), "cols", 6 if j >= DIRECT else 4)
        cols = pl.ds(pl.multiple_of(at_z(spots[j]) * 256, 256), 256)
        total = (
            last[j, g, 0].astype(F32)
            + last_in[j, g, 0].astype(F32)
            + last_in[j, g, 1].astype(F32)
        )
        if j >= DIRECT:
            total += far_in[j - DIRECT, g].astype(F32)
        out_ref[pl.ds(g * half, half), cols] = (middle[g, :, cols] + total).astype(BF16)

    halo()
    for copy in own_up:
        copy.wait()
    z_hop("u", 0)
    own_gate.wait()
    gate_start()
    send_x("u", 0)
    gate_hop(0, 0)
    q_copy.wait()
    attend_early()
    attend_second()
    own_down.wait()
    z_hop("d", 0)
    wait_halos()
    attend_third()
    wo_copy.wait()
    z_hop("u", 1)
    send_x("u", 1)
    send_x("u", 2)
    project(3)
    gate_relay()
    attend_late()
    gate_hop(1, 0)
    project(1)
    relay_x("u", 0)
    gate_hop(-1, 0)
    project(2)
    first_near(0)
    project(0)
    gate_hop(0, 1)
    relay_x("u", 1)
    z_hop("u", 2)
    send_x("u", 3)
    send_x("u", 4)
    relay_x("u", 2)
    gate_close()
    gate_hop(2, 0)
    gate_twin(0)
    pass_first(0)
    first_near(1)
    close_x("u", 0)
    pass_first(1)
    gate_hop(1, 1)
    close_x("u", 1)
    gate_hop(-1, 1)
    relay_x("u", 3)
    z_hop("u", 3)
    send_x("u", 5)
    send_x("u", 6)
    relay_x("u", 4)
    norm(0)
    gate_hop(0, 2)
    close_x("u", 2)
    close_x("u", 3)
    gate_hop(2, 1)
    gate_twin(1)
    gate_hop(1, 2)
    relay_x("u", 5)
    z_hop("u", 4)
    send_x("u", 7)
    gate_hop(-1, 2)
    relay_x("u", 6)
    close_x("u", 4)
    gate_hop(0, 3)
    close_x("u", 5)
    send_x("d", 0)
    spread_relay(0)
    norm(1)
    gate_hop(2, 2)
    gate_twin(2)
    z_hop("d", 1)
    send_x("d", 1)
    relay_x("u", 7)
    close_x("u", 6)
    gate_hop(1, 3)
    gate_hop(-1, 3)
    gate_hop(0, 4)
    send_x("d", 2)
    relay_x("d", 0)
    spread_end(0)
    gate_hop(2, 3)
    gate_twin(3)
    relay_x("d", 1)
    close_x("u", 7)
    z_hop("d", 2)
    spread_relay(1)
    send_x("d", 3)
    gate_hop(1, 4)
    relay_x("d", 2)
    gate_hop(-1, 4)
    wait_twins("u")
    expand_up(0, 0, 3)
    gate_hop(2, 4)
    gate_twin(4)
    close_x("d", 0)
    expand_up(0, 3, 2)
    expand_tail(0)
    send_x("d", 4)
    close_x("d", 1)
    z_hop("d", 3)
    wait_twins("g")
    expand_gate(0, 0, 2)
    spread_end(1)
    relay_x("d", 3)
    expand_gate(0, 2, 3)
    send_x("d", 5)
    close_x("d", 2)
    contract(0, 0)
    contract(1, 0)
    z_hop("d", 4)
    expand_up(1, 0, 3)
    relay_x("d", 4)
    contract(2, 0)
    send_x("d", 6)
    close_x("d", 3)
    expand_up(1, 3, 2)
    expand_tail(1)
    pass_last(0, 0)
    expand_gate(1, 0, 2)
    pass_last(1, 0)
    relay_x("d", 5)
    expand_gate(1, 2, 3)
    pass_last(2, 0)
    send_x("d", 7)
    close_x("d", 4)
    contract(3, 0)
    contract(0, 1)
    contract(1, 1)
    relay_x("d", 6)
    contract(2, 1)
    contract(4, 0)
    close_x("d", 5)
    contract(3, 1)
    pass_last(3, 0)
    contract(4, 1)
    pass_last(0, 1)
    finish(0, 0)
    finish(1, 0)
    finish(2, 0)
    relay_x("d", 7)
    pass_last(1, 1)
    contract(5, 0)
    pass_last(2, 1)
    close_x("d", 6)
    contract(5, 1)
    pass_last(4, 0)
    pass_last(3, 1)
    finish(3, 0)
    pass_last(4, 1)
    close_x("d", 7)
    contract(6, 0)
    contract(6, 1)
    pass_last(5, 0)
    finish(0, 1)
    finish(1, 1)
    finish(2, 1)
    contract(7, 0)
    pass_last(5, 1)
    contract(7, 1)
    finish(4, 0)
    finish(3, 1)
    finish(4, 1)
    pass_last(6, 0)
    pass_last(6, 1)
    finish(5, 0)
    finish(7, 0)
    finish(5, 1)
    finish(7, 1)
    finish(6, 0)
    finish(6, 1)
    wait_sent()
    assert (len(sent), len(arriving)) == (N_SENT, N_ARRIVING)


def shards(
    queries,
    key_rows,
    value_rows,
    sink_logits,
    residual,
    norm_gain,
    out_weight,
    gate_weight,
    up_weight,
    down_weight,
):
    tok, width = queries.shape
    d = residual.shape[1]
    rows, ff = gate_weight.shape
    share = tok // 4
    half = share // 2
    gate_part, up_part, down_part = (
        pltpu.VMEM((ZN, XN, CN, rows, columns), BF16) for columns in (ff - TAIL, ff + TAIL, ff)
    )
    narrow = d // LAST_CHUNKS
    hbm = pl.BlockSpec(memory_space=pl.ANY)
    smem = pl.BlockSpec(memory_space=pltpu.SMEM)
    return pl.pallas_call(
        functools.partial(body, tok * lax.axis_size("sp")),
        out_shape=pltpu.VMEM((share, d), BF16),
        in_specs=[hbm, hbm, hbm, smem, hbm, hbm, hbm, hbm, hbm, hbm],
        out_specs=pl.BlockSpec(memory_space=pltpu.VMEM),
        scratch_shapes=[
            pltpu.VMEM((tok, width), BF16),
            pltpu.VMEM((tok + 2 * WIN, DH), BF16),
            pltpu.VMEM((tok + 2 * WIN, DH), BF16),
            pltpu.VMEM((share, d), BF16),
            pltpu.VMEM((1, d), F32),
            pltpu.VMEM((width, d), BF16),
            gate_part,
            up_part,
            down_part,
            pltpu.VMEM((tok, width), BF16),
            pltpu.VMEM((2, 4, half, d), BF16),
            pltpu.VMEM((2, 2, half // 2, d), BF16),
            pltpu.VMEM((2, 2, half, d), BF16),
            pltpu.VMEM((2, half, d), F32),
            pltpu.VMEM((2, 4, half, d), BF16),
            pltpu.VMEM((2, tok // 2, ff - TAIL), F32),
            pltpu.VMEM((2, tok // 2, ff), BF16),
            pltpu.VMEM((LAST_CHUNKS, 2, 4, half, narrow), BF16),
            pltpu.VMEM((LAST_CHUNKS, 2, 2, half // 2, narrow), BF16),
            pltpu.VMEM((LAST_CHUNKS, 2, 2, half, narrow), BF16),
            pltpu.VMEM((LAST_CHUNKS - DIRECT, 2, half, narrow), BF16),
            pltpu.SemaphoreType.DMA((N_SENT,)),
            pltpu.SemaphoreType.DMA((N_ARRIVING,)),
            pltpu.SemaphoreType.DMA((10,)),
        ],
        compiler_params=pltpu.CompilerParams(
            collective_id=0, has_side_effects=True, vmem_limit_bytes=67043328 - 2**19
        ),
        name="layer",
    )(
        queries,
        key_rows,
        value_rows,
        sink_logits,
        residual,
        norm_gain.reshape(1, d),
        out_weight,
        gate_weight,
        up_weight,
        down_weight.T,
    )


def solution(mesh):
    placed = (
        P("sp", "tp"),
        P("sp", "tp"),
        P("sp", "tp"),
        P("tp"),
        P("sp", None),
        P(),
        P("tp", None),
        P("sp", "tp"),
        P("sp", "tp"),
        P("tp", "sp"),
    )
    return jax.shard_map(
        shards, mesh=mesh, in_specs=placed, out_specs=P(("sp", "tp"), None), check_vma=False
    )
```
